32 devices in a mesh: ep: 8 (over z, core), tp: 4 (over y, x).
Axes of the slice: x: 2, y: 2, z: 4, core: 2. Of those that a mesh axis runs over, the one named last changes fastest.
Arguments:
- tokens: bfloat16 [1024, 2048], P('ep', 'tp'), may hold values from -3000 to 3000
- norm_gain: float32 [2048], replicated, may hold values from 0.1 to 1.9
- gate_weight: bfloat16 [8, 2048, 512], P('ep'), may hold values from -0.125 to 0.125
- up_weight: bfloat16 [8, 2048, 512], P('ep'), may hold values from -0.125 to 0.125
- down_weight: bfloat16 [8, 512, 2048], P('ep'), may hold values from -0.25 to 0.25
- expert_ids: int32 [1024, 2], P('ep'), may hold values from 0 to 7, as said below
- route_weight: float32 [1024, 2], P('ep'), may hold values from 0.2 to 1
Outputs:
- mixed: bfloat16 [1024, 2048], P('ep', 'tp')
The draws below stay inside these ranges and needn't reach their ends.
Inputs may be any that keep to these rules, and one draw needn't show every extreme that they name: `expert_ids`: A token's two experts differ and lie in one group of 2 consecutive experts. In each aligned block of 32 rows no expert is named more than 16 times, and in every block all experts of one group, the same group for all blocks, are named exactly 16 times.
All inputs are finite; a program needn't handle non-finite values.
Results may differ from the reference program's by a relative error of at most 0.0071.
Values may be sent and summed in bfloat16 or wider, within the bound.
No kernel may reach another device: no remote copies, remote signals or barrier semaphores. Data moves between devices by JAX's collectives and lax.ppermute only.
A program may use at most 64 MiB of HBM per device.

```python
import math
import jax
import jax.numpy as jnp
from jax import lax

D = 2048
FF = 512
TOK_DEV = 32
EXPERTS = 8
EPG = 2
GROUPS = 4
CAP = 16
GCAP = 16
TOKENS = 1024


def group_order(order_key):
    return jax.random.permutation(order_key, EPG)


def route_block(block_key, hot_group):
    keys = jax.random.split(block_key, 5)
    group_bias = jax.random.randint(keys[0], (GROUPS,), 1, 5)
    slot_group = jnp.arange(GROUPS * GCAP, dtype=jnp.int32) // GCAP
    score = jax.random.randint(keys[1], (GROUPS * GCAP,), 0, 65536) * group_bias[slot_group]
    score = jnp.where(slot_group == hot_group, 4194304, score)
    score = score * (GROUPS * GCAP) + jnp.arange(GROUPS * GCAP, dtype=jnp.int32)
    unused, chosen = lax.top_k(score, TOK_DEV)
    chosen = chosen[jax.random.permutation(keys[2], TOK_DEV)]
    group_of = chosen // GCAP
    within = chosen % GCAP
    orders = jax.vmap(group_order)(jax.random.split(keys[3], GROUPS))
    offsets = jax.random.randint(keys[4], (GROUPS, CAP // 2), 1, EPG)
    position = within % EPG
    first = orders[group_of, position]
    second = orders[group_of, (position + offsets[group_of, within // EPG]) % EPG]
    return jnp.stack([group_of * EPG + first, group_of * EPG + second], axis=1).astype(jnp.int32)


def draw_expert_ids(key, part):
    hot_group = jax.random.randint(jax.random.fold_in(key, 11), (), 0, GROUPS)
    block_keys = jax.random.split(jax.random.fold_in(key, 12), TOKENS // TOK_DEV)
    blocks = jax.vmap(route_block, in_axes=(0, None))(block_keys, hot_group)
    return blocks.reshape(TOKENS, 2)


def draw_tokens(key, part):
    keys = jax.random.split(jax.random.fold_in(key, 21), 4)
    column_rise = jnp.exp(jnp.log(10.0) * jnp.arange(D, dtype=jnp.float32) / D)
    column_rough = jnp.exp(jax.random.uniform(keys[0], (D,), jnp.float32, -0.5, 0.5))
    row_scale = jnp.exp(jax.random.uniform(keys[1], (TOKENS, 1), jnp.float32, 0.0, jnp.log(10.0)))
    base = jnp.clip(jax.random.normal(keys[3], (TOKENS, D), jnp.float32), -6.0, 6.0)
    return (base * row_scale * column_rise * column_rough).astype(jnp.bfloat16)


def shard_levels(stream_key, extent, shards, low, largest):
    loudness = 1.0
    for dim, parts in shards:
        steps = jax.random.uniform(jax.random.fold_in(jax.random.fold_in(stream_key, 6), dim), (parts,), jnp.float32, low / len(shards), largest / len(shards))
        loudness = loudness * jnp.repeat(jnp.exp(steps), extent[dim] // parts).reshape((-1,) + (1,) * (len(extent) - 1 - dim))
    return loudness


def centred(stream_key, extent, deviation, reach, cuts=(), held_as=jnp.bfloat16):
    array = jax.random.normal(stream_key, extent, jnp.float32) * deviation
    if len(cuts) > 0:
        array = shard_levels(stream_key, extent, cuts, -0.22, 0.18) * array
    return jnp.clip(array, min=-reach, max=reach).astype(held_as)


def setup_inputs(seed: int = 0) -> dict:
    key_of = jax.random.split(jax.random.key(seed), 8)
    tokens = draw_tokens(jax.random.fold_in(key_of[7], 71), 0)
    norm_gain = jnp.clip(1.0 + 0.18 * jax.random.normal(key_of[1], (D,), jnp.float32), 0.1, 1.9)
    gate_weight = centred(key_of[2], (EXPERTS, D, FF), D ** -0.5, 0.125, ((0, 8),))
    up_weight = centred(key_of[3], (EXPERTS, D, FF), D ** -0.5, 0.125, ((0, 8),))
    down_weight = centred(key_of[4], (EXPERTS, FF, D), FF ** -0.5, 0.25, ((0, 8),))
    expert_ids = draw_expert_ids(jax.random.fold_in(key_of[7], 71), 0)
    route_weight = jnp.clip(jnp.exp(math.log(1.0) - 1.609438 * jax.random.uniform(key_of[6], (TOKENS, 2), jnp.float32) ** shard_levels(key_of[6], (TOKENS, 2), ((0, 8),), -0.2, 0.2)), 0.2, 1.0)
    return {"tokens": tokens, "norm_gain": norm_gain, "gate_weight": gate_weight, "up_weight": up_weight, "down_weight": down_weight, "expert_ids": expert_ids, "route_weight": route_weight}


def reference(tokens, norm_gain, gate_weight, up_weight, down_weight, expert_ids, route_weight):
    widened = tokens.astype(jnp.float32)
    mean_square = lax.optimization_barrier(jnp.mean(widened * widened, axis=-1, keepdims=True))
    normed = (widened * lax.rsqrt(mean_square + 1e-06) * norm_gain).astype(jnp.bfloat16)
    flat_ids = expert_ids.reshape(-1)
    flat_weight = route_weight.reshape(-1)
    longest = TOKENS // TOK_DEV * CAP

    def per_expert(summed, expert):
        matches = flat_ids == expert
        places = jnp.nonzero(matches, size=longest, fill_value=0)[0].astype(jnp.int32)
        present = jnp.arange(longest, dtype=jnp.int32) < jnp.sum(matches.astype(jnp.int32))
        token_rows = places // 2
        chosen = normed[token_rows]
        gate_part = jnp.dot(chosen, gate_weight[expert], preferred_element_type=jnp.float32)
        up_part = jnp.dot(chosen, up_weight[expert], preferred_element_type=jnp.float32)
        hidden = (jax.nn.silu(gate_part) * up_part).astype(jnp.bfloat16)
        produced = jnp.dot(hidden, down_weight[expert], preferred_element_type=jnp.float32).astype(jnp.bfloat16)
        produced = lax.optimization_barrier(produced).astype(jnp.float32)
        weight_used = jnp.where(present, flat_weight[places], 0.0)
        summed = summed.at[token_rows].add(produced * weight_used[:, None])
        return (summed, None)
    summed, unused = lax.scan(per_expert, jnp.zeros((TOKENS, D), jnp.float32), jnp.arange(EXPERTS, dtype=jnp.int32))
    return summed.astype(jnp.bfloat16)
```

```python
from functools import partial

import jax
import jax.numpy as jnp
from jax import lax
from jax.experimental import pallas as pl
from jax.experimental.pallas import tpu as pltpu
from jax.sharding import PartitionSpec as P


F32 = jnp.float32
BF16 = jnp.bfloat16
LANES = 128
VMEM = pl.BlockSpec(memory_space=pltpu.VMEM)


def slot_numbers(block_ids, experts):
    flat_ids = block_ids.reshape(-1)
    hit_table = (flat_ids[:, None] == jnp.arange(experts, dtype=jnp.int32)[None, :]).astype(
        jnp.int32
    )
    earlier = jnp.cumsum(hit_table, axis=0) - hit_table
    return (flat_ids, jnp.sum(earlier * hit_table, axis=1))


def placement_matrix(flat_ids, slot_index, experts, capacity):
    target = (flat_ids * capacity + slot_index).reshape(-1, 2)
    slot_rows = jnp.arange(experts * capacity, dtype=jnp.int32)[:, None]
    first_hit = (target[:, 0][None, :] == slot_rows).astype(BF16)
    second_hit = (target[:, 1][None, :] == slot_rows).astype(BF16)
    return first_hit + second_hit


def expert_apply(row_data, gate_weight, up_weight, down_weight):
    shape_in = row_data.shape
    flat_rows = row_data.reshape(-1, shape_in[-1])
    gate_part = jnp.dot(flat_rows, gate_weight[0], preferred_element_type=F32)
    up_part = jnp.dot(flat_rows, up_weight[0], preferred_element_type=F32)
    hidden = (jax.nn.silu(gate_part) * up_part).astype(BF16)
    produced = jnp.dot(hidden, down_weight[0], preferred_element_type=F32).astype(BF16)
    return produced.reshape(shape_in[:-1] + (produced.shape[-1],))


def local_any(tokens, norm_gain, gate_weight, up_weight, down_weight, expert_ids, route_weight):
    tp_count = lax.axis_size("tp")
    experts = lax.axis_size("ep") * gate_weight.shape[0]
    model_width = gate_weight.shape[1]
    group_rows = tokens.shape[0]
    block_rows = group_rows // tp_count
    capacity = 4 * block_rows // experts
    tp_index = lax.axis_index("tp")
    apply_experts = partial(
        expert_apply, gate_weight=gate_weight, up_weight=up_weight, down_weight=down_weight
    )
    full_rows = lax.all_to_all(tokens, "tp", split_axis=0, concat_axis=1, tiled=True)
    block_ids = lax.dynamic_slice_in_dim(expert_ids, tp_index * block_rows, block_rows, 0)
    block_weight = lax.dynamic_slice_in_dim(route_weight, tp_index * block_rows, block_rows, 0)
    widened = full_rows.astype(F32)
    mean_square = jnp.mean(widened * widened, axis=-1, keepdims=True)
    normed = (widened * lax.rsqrt(mean_square + 1e-06) * norm_gain).astype(BF16)
    flat_ids, slot_index = slot_numbers(block_ids, experts)
    placing = placement_matrix(flat_ids, slot_index, experts, capacity)
    outgoing = jnp.dot(placing, normed, preferred_element_type=F32).astype(BF16)
    outgoing = outgoing.reshape(experts, capacity, model_width)
    produced = apply_experts(
        lax.all_to_all(outgoing, "ep", split_axis=0, concat_axis=0, tiled=True)
    )
    returned = lax.all_to_all(produced, "ep", split_axis=0, concat_axis=0, tiled=True)
    picked = jnp.take(returned.reshape(-1, model_width), flat_ids * capacity + slot_index, axis=0)
    weighted = picked.astype(F32) * block_weight.reshape(-1)[:, None]
    mixed_rows = weighted.reshape(block_rows, 2, model_width).sum(axis=1).astype(BF16)
    return lax.all_to_all(mixed_rows, "tp", split_axis=1, concat_axis=0, tiled=True)


def routing_kernel(
    groups, capacity, ids_ref, weight_ref, gain_in_ref, place_ref, code_ref, gain_ref
):
    gain_ref[...] = gain_in_ref[...]
    me = lax.axis_index("ep")
    chip, core = me // 2, me % 2
    rows = ids_ref.shape[1]
    slots = groups * capacity
    first = ids_ref[0:1, :]
    relative = (first >> 1) ^ chip
    hot = (relative == lax.broadcasted_iota(jnp.int32, (groups, rows), 0)).astype(F32)
    before = (
        lax.broadcasted_iota(jnp.int32, (rows, rows), 0)
        < lax.broadcasted_iota(jnp.int32, (rows, rows), 1)
    ).astype(F32)
    rank = jnp.dot(hot, before, preferred_element_type=F32)
    position = lax.broadcasted_iota(jnp.int32, (capacity, rows), 0).astype(F32)
    place = jnp.concatenate(
        [
            jnp.where(rank[k : k + 1] == position, 1.0, 0.0) * hot[k : k + 1]
            for k in range(groups)
        ],
        axis=0,
    )
    place_ref[...] = place.astype(BF16)
    mine = (first & 1) == core
    lane = lax.broadcasted_iota(jnp.int32, (slots, LANES), 1)
    code = jnp.zeros((slots, LANES), F32)
    for which, row in enumerate(
        (
            jnp.where(mine, weight_ref[0:1, :], weight_ref[1:2, :]),
            jnp.where(mine, weight_ref[1:2, :], weight_ref[0:1, :]),
        )
    ):
        rest = jnp.sum(place * row, axis=1, keepdims=True)
        for part in range(3):
            piece = rest.astype(BF16).astype(F32)
            rest = rest - piece
            code = jnp.where(lane == 3 * which + part, piece, code)
    code_ref[...] = code.astype(BF16)


def dispatch_kernel(count, groups, capacity, *refs):
    parts, (gain_ref, place_ref, code_ref), outs = refs[:count], refs[count : count + 3], refs[count + 3 :]
    me = lax.axis_index("tp")
    width = parts[0].shape[1]
    wide = [p[...].astype(F32) for p in parts]
    square = sum(jnp.sum(w * w, axis=1, keepdims=True) for w in wide)
    scale = lax.rsqrt(square / (width * count) + 1e-06)
    place = place_ref[...]
    for k in range(count):
        at = pl.ds(pl.multiple_of((me ^ k) * width, width), width)
        normed = (wide[k] * scale * gain_ref[:, at]).astype(BF16)
        placed = jnp.dot(place, normed, preferred_element_type=F32).astype(BF16)
        for g in range(groups):
            outs[g][:, at] = placed[g * capacity : (g + 1) * capacity]
    for g in range(groups):
        outs[g][:, width * count :] = code_ref[g * capacity : (g + 1) * capacity, :]


def expert_kernel(groups, width, *refs):
    rows, weights, outs = refs[:groups], refs[groups : groups + 6], refs[groups + 6 :]
    x = jnp.concatenate([r[:, :width] for r in rows], axis=0)
    code = jnp.concatenate([r[:, width:] for r in rows], axis=0).astype(F32)
    total = None
    for which in range(2):
        gate_ref, up_ref, down_ref = weights[3 * which : 3 * which + 3]
        gate = jnp.dot(x, gate_ref[0], preferred_element_type=F32)
        up = jnp.dot(x, up_ref[0], preferred_element_type=F32)
        hidden = (gate / (1.0 + jnp.exp(-gate)) * up).astype(BF16)
        made = jnp.dot(hidden, down_ref[0], preferred_element_type=F32).astype(BF16)
        at = 3 * which
        weight = code[:, at : at + 1] + code[:, at + 1 : at + 2] + code[:, at + 2 : at + 3]
        term = made.astype(F32) * weight
        total = term if total is None else total + term
    mixed = total.astype(BF16)
    capacity = rows[0].shape[0]
    for g in range(groups):
        outs[g][...] = mixed[g * capacity : (g + 1) * capacity]


def restore_kernel(count, groups, *refs):
    rows, place_ref, outs = refs[:groups], refs[groups], refs[groups + 1 :]
    me = lax.axis_index("tp")
    width = outs[0].shape[1]
    back = place_ref[...].astype(F32).T.astype(BF16)
    for k in range(count):
        at = pl.ds(pl.multiple_of((me ^ k) * width, width), width)
        got = jnp.concatenate([r[:, at] for r in rows], axis=0)
        outs[k][...] = jnp.dot(back, got, preferred_element_type=F32).astype(BF16)


def assemble_kernel(count, *refs):
    parts, out_ref = refs[:count], refs[count]
    me = lax.axis_index("tp")
    rows = parts[0].shape[0]
    for k in range(count):
        out_ref[pl.ds(pl.multiple_of((me ^ k) * rows, rows), rows), :] = parts[k][...]


def call(kernel, outs, args, flops, limit=4 << 20):
    return pl.pallas_call(
        kernel,
        out_shape=outs,
        in_specs=[VMEM] * len(args),
        out_specs=jax.tree.map(lambda _: VMEM, outs),
        compiler_params=pltpu.CompilerParams(vmem_limit_bytes=limit),
        cost_estimate=pl.CostEstimate(flops=flops, bytes_accessed=1 << 20, transcendentals=0),
    )(*args)


def exchange(array, axis, size, mask):
    return lax.ppermute(array, axis, [(i, i ^ mask) for i in range(size)])


def exchange_all(pieces, axis, size, stride):
    got = {0: pieces[0]}
    for k in range(1, len(pieces)):
        got[k] = exchange(pieces[k], axis, size, stride * k)
    return [got[k] for k in range(len(pieces))]


def local_pairs(tokens, norm_gain, gate_weight, up_weight, down_weight, expert_ids, route_weight):
    tp_count = lax.axis_size("tp")
    ep_count = lax.axis_size("ep")
    groups = ep_count // 2
    width = gate_weight.shape[1]
    part = tokens.shape[1]
    block = tokens.shape[0] // tp_count
    capacity = 4 * block // ep_count
    slots = groups * capacity
    tp_index = lax.axis_index("tp")
    weights = (gate_weight, up_weight, down_weight)

    mine = [
        lax.dynamic_slice_in_dim(tokens, (tp_index ^ k) * block, block, 0) for k in range(tp_count)
    ]
    parts = exchange_all(mine, "tp", tp_count, 1)
    others = []
    for w in weights:
        others.append(exchange(w, "ep", ep_count, 1))

    ids = lax.dynamic_slice_in_dim(expert_ids.T, tp_index * block, block, 1)
    route = lax.dynamic_slice_in_dim(route_weight.T, tp_index * block, block, 1)
    place, code, gain = call(
        partial(routing_kernel, groups, capacity),
        (
            jax.ShapeDtypeStruct((slots, block), BF16),
            jax.ShapeDtypeStruct((slots, LANES), BF16),
            jax.ShapeDtypeStruct((1, width), F32),
        ),
        (ids, route, norm_gain.reshape(1, -1)),
        1 << 33,
    )
    row = jax.ShapeDtypeStruct((capacity, width + LANES), BF16)
    sent = call(
        partial(dispatch_kernel, tp_count, groups, capacity),
        (row,) * groups,
        (*parts, gain, place, code),
        1 << 24,
    )
    arrived = exchange_all(sent, "ep", ep_count, 2)
    made = call(
        partial(expert_kernel, groups, width),
        (jax.ShapeDtypeStruct((capacity, width), BF16),) * groups,
        (*arrived, *weights, *others),
        1 << 30,
        8 << 20,
    )
    returned = exchange_all(made, "ep", ep_count, 2)
    slices = call(
        partial(restore_kernel, tp_count, groups),
        (jax.ShapeDtypeStruct((block, part), BF16),) * tp_count,
        (*returned, place),
        1 << 24,
    )
    final = exchange_all(slices, "tp", tp_count, 1)
    return call(
        partial(assemble_kernel, tp_count),
        jax.ShapeDtypeStruct(tokens.shape, BF16),
        final,
        1 << 20,
    )


def solution(mesh):
    in_specs = (
        P("ep", "tp"),
        P(),
        P("ep", None, None),
        P("ep", None, None),
        P("ep", None, None),
        P("ep", None),
        P("ep", None),
    )
    group_experts = mesh.shape["tp"] // 2
    pairs = group_experts == 2

    def body(*arrays):
        return (local_pairs if pairs else local_any)(*arrays)

    return jax.shard_map(
        body, mesh=mesh, in_specs=in_specs, out_specs=P("ep", "tp"), check_vma=False
    )
```

```python
from functools import partial

import jax
import jax.numpy as jnp
from jax import lax
from jax.experimental import pallas as pl
from jax.experimental.pallas import tpu as pltpu
from jax.sharding import PartitionSpec as P


F32 = jnp.float32
BF16 = jnp.bfloat16
LANES = 128
VMEM = pl.BlockSpec(memory_space=pltpu.VMEM)


def slot_numbers(block_ids, experts):
    flat_ids = block_ids.reshape(-1)
    hit_table = (flat_ids[:, None] == jnp.arange(experts, dtype=jnp.int32)[None, :]).astype(
        jnp.int32
    )
    earlier = jnp.cumsum(hit_table, axis=0) - hit_table
    return (flat_ids, jnp.sum(earlier * hit_table, axis=1))


def placement_matrix(flat_ids, slot_index, experts, capacity):
    target = (flat_ids * capacity + slot_index).reshape(-1, 2)
    slot_rows = jnp.arange(experts * capacity, dtype=jnp.int32)[:, None]
    first_hit = (target[:, 0][None, :] == slot_rows).astype(BF16)
    second_hit = (target[:, 1][None, :] == slot_rows).astype(BF16)
    return first_hit + second_hit


def expert_apply(row_data, gate_weight, up_weight, down_weight):
    shape_in = row_data.shape
    flat_rows = row_data.reshape(-1, shape_in[-1])
    gate_part = jnp.dot(flat_rows, gate_weight[0], preferred_element_type=F32)
    up_part = jnp.dot(flat_rows, up_weight[0], preferred_element_type=F32)
    hidden = (jax.nn.silu(gate_part) * up_part).astype(BF16)
    produced = jnp.dot(hidden, down_weight[0], preferred_element_type=F32).astype(BF16)
    return produced.reshape(shape_in[:-1] + (produced.shape[-1],))


def local_any(tokens, norm_gain, gate_weight, up_weight, down_weight, expert_ids, route_weight):
    tp_count = lax.axis_size("tp")
    experts = lax.axis_size("ep") * gate_weight.shape[0]
    model_width = gate_weight.shape[1]
    group_rows = tokens.shape[0]
    block_rows = group_rows // tp_count
    capacity = 4 * block_rows // experts
    tp_index = lax.axis_index("tp")
    apply_experts = partial(
        expert_apply, gate_weight=gate_weight, up_weight=up_weight, down_weight=down_weight
    )
    full_rows = lax.all_to_all(tokens, "tp", split_axis=0, concat_axis=1, tiled=True)
    block_ids = lax.dynamic_slice_in_dim(expert_ids, tp_index * block_rows, block_rows, 0)
    block_weight = lax.dynamic_slice_in_dim(route_weight, tp_index * block_rows, block_rows, 0)
    widened = full_rows.astype(F32)
    mean_square = jnp.mean(widened * widened, axis=-1, keepdims=True)
    normed = (widened * lax.rsqrt(mean_square + 1e-06) * norm_gain).astype(BF16)
    flat_ids, slot_index = slot_numbers(block_ids, experts)
    placing = placement_matrix(flat_ids, slot_index, experts, capacity)
    outgoing = jnp.dot(placing, normed, preferred_element_type=F32).astype(BF16)
    outgoing = outgoing.reshape(experts, capacity, model_width)
    produced = apply_experts(
        lax.all_to_all(outgoing, "ep", split_axis=0, concat_axis=0, tiled=True)
    )
    returned = lax.all_to_all(produced, "ep", split_axis=0, concat_axis=0, tiled=True)
    picked = jnp.take(returned.reshape(-1, model_width), flat_ids * capacity + slot_index, axis=0)
    weighted = picked.astype(F32) * block_weight.reshape(-1)[:, None]
    mixed_rows = weighted.reshape(block_rows, 2, model_width).sum(axis=1).astype(BF16)
    return lax.all_to_all(mixed_rows, "tp", split_axis=1, concat_axis=0, tiled=True)


def routing_kernel(
    groups, capacity, block, ids_ref, place_ref, wide_ref, back_ref, first_ref
):
    chip = lax.axis_index("ep") // 2
    column = lax.axis_index("tp")
    rows = ids_ref.shape[1]
    columns = rows // block
    first = ids_ref[0:1, :]
    first_ref[...] = first
    group = first >> 1
    bin_of = group * columns + lax.broadcasted_iota(jnp.int32, (1, rows), 1) // block
    bins = groups * columns
    hot = bin_of == lax.broadcasted_iota(jnp.int32, (bins, rows), 0)
    before = lax.broadcasted_iota(jnp.int32, (rows, rows), 0) < lax.broadcasted_iota(
        jnp.int32, (rows, rows), 1
    )
    ahead = jnp.dot(
        hot.astype(F32).astype(BF16), before.astype(F32).astype(BF16), preferred_element_type=F32
    )
    rank = jnp.sum(jnp.where(hot, ahead, 0.0), axis=0, keepdims=True)
    position = lax.broadcasted_iota(jnp.int32, (capacity, rows), 0).astype(F32)
    at = rank == position

    def placed(which):
        return jnp.where(at & (bin_of == which), 1.0, 0.0)

    full = jnp.concatenate([placed(n) for n in range(bins)], axis=0)
    back_ref[...] = full.T.astype(BF16)
    wide = jnp.concatenate(
        [placed((k ^ chip) * columns + column) for k in range(groups)], axis=0
    )
    wide_ref[...] = wide.astype(BF16)
    place_ref[...] = pltpu.roll(wide, rows - column * block, 1)[:, :block].astype(BF16)


def code_of(wide, first, route, core):
    mine = (first & 1) == core
    lane = lax.broadcasted_iota(jnp.int32, (wide.shape[0], LANES), 1)
    code = jnp.zeros(lane.shape, F32)
    for which in range(2):
        row = jnp.where(mine, route[which : which + 1], route[1 - which : 2 - which])
        rest = jnp.sum(wide * row, axis=1, keepdims=True)
        for part in range(3):
            piece = rest.astype(BF16).astype(F32)
            rest = rest - piece
            code = jnp.where(lane == 3 * which + part, piece, code)
    return code.astype(BF16)


def dispatch_kernel(count, groups, capacity, *refs):
    parts, (gain_ref, place_ref, wide_ref, first_ref, route_ref), outs = (
        refs[:count],
        refs[count : count + 5],
        refs[count + 5 :],
    )
    me = lax.axis_index("tp")
    core = lax.axis_index("ep") % 2
    width = parts[0].shape[1]
    code = code_of(wide_ref[...].astype(F32), first_ref[...], route_ref[...], core)
    wide = [p[...].astype(F32) for p in parts]
    square = sum(jnp.sum(w * w, axis=1, keepdims=True) for w in wide)
    scale = lax.rsqrt(square / (width * count) + 1e-06)
    place = place_ref[...]
    for k in range(count):
        at = pl.ds(pl.multiple_of((me ^ k) * width, width), width)
        normed = (wide[k] * scale * gain_ref[:, at]).astype(BF16)
        placed = jnp.dot(place, normed, preferred_element_type=F32).astype(BF16)
        for g in range(groups):
            outs[g][:, at] = placed[g * capacity : (g + 1) * capacity]
    for g in range(groups):
        outs[g][:, width * count :] = code[g * capacity : (g + 1) * capacity]


def expert_kernel(groups, width, *refs):
    rows, weights, out_ref = refs[:groups], refs[groups : groups + 6], refs[groups + 6]
    x = jnp.concatenate([r[:, :width] for r in rows], axis=0)
    code = jnp.concatenate([r[:, width:] for r in rows], axis=0).astype(F32)
    total = None
    for which in range(2):
        gate_ref, up_ref, down_ref = weights[3 * which : 3 * which + 3]
        gate = jnp.dot(x, gate_ref[0], preferred_element_type=F32)
        up = jnp.dot(x, up_ref[0], preferred_element_type=F32)
        hidden = (gate / (1.0 + jnp.exp(-gate)) * up).astype(BF16)
        made = jnp.dot(hidden, down_ref[0], preferred_element_type=F32).astype(BF16)
        at = 3 * which
        weight = code[:, at : at + 1] + code[:, at + 1 : at + 2] + code[:, at + 2 : at + 3]
        term = made.astype(F32) * weight
        total = term if total is None else total + term
    mixed = total.astype(BF16)
    chip = lax.axis_index("ep") // 2
    capacity, part = out_ref.shape[1:]
    columns = width // part
    for g in range(groups):
        for n in range(columns):
            out_ref[(g ^ chip) * columns + n] = mixed[
                g * capacity : (g + 1) * capacity, n * part : (n + 1) * part
            ]


def restore_kernel(rows_ref, back_ref, out_ref):
    rows = rows_ref[...].reshape(-1, rows_ref.shape[-1])
    out_ref[...] = jnp.dot(back_ref[...], rows, preferred_element_type=F32).astype(BF16)


def call(kernel, outs, args, flops, limit=4 << 20):
    return pl.pallas_call(
        kernel,
        out_shape=outs,
        in_specs=[VMEM] * len(args),
        out_specs=jax.tree.map(lambda _: VMEM, outs),
        compiler_params=pltpu.CompilerParams(vmem_limit_bytes=limit),
        cost_estimate=pl.CostEstimate(flops=flops, bytes_accessed=1 << 20, transcendentals=0),
    )(*args)


def exchange(array, axis, size, mask):
    return lax.ppermute(array, axis, [(i, i ^ mask) for i in range(size)])


def exchange_all(pieces, axis, size, stride):
    got = {0: pieces[0]}
    for k in range(1, len(pieces)):
        got[k] = exchange(pieces[k], axis, size, stride * k)
    return [got[k] for k in range(len(pieces))]


def local_pairs(tokens, norm_gain, gate_weight, up_weight, down_weight, expert_ids, route_weight):
    tp_count = lax.axis_size("tp")
    ep_count = lax.axis_size("ep")
    groups = ep_count // 2
    width = gate_weight.shape[1]
    part = tokens.shape[1]
    all_rows = tokens.shape[0]
    block = all_rows // tp_count
    capacity = 4 * block // ep_count
    slots = groups * capacity
    tp_index = lax.axis_index("tp")
    weights = (gate_weight, up_weight, down_weight)

    mine = [
        lax.dynamic_slice_in_dim(tokens, (tp_index ^ k) * block, block, 0) for k in range(tp_count)
    ]
    parts = exchange_all(mine, "tp", tp_count, 1)
    others = []
    for w in weights:
        others.append(exchange(w, "ep", ep_count, 1))

    ids, route = expert_ids.T, route_weight.T
    bins = groups * tp_count
    place, wide, back, first = call(
        partial(routing_kernel, groups, capacity, block),
        (
            jax.ShapeDtypeStruct((slots, block), BF16),
            jax.ShapeDtypeStruct((slots, all_rows), BF16),
            jax.ShapeDtypeStruct((all_rows, bins * capacity), BF16),
            jax.ShapeDtypeStruct((1, all_rows), jnp.int32),
        ),
        (ids,),
        1 << 33,
    )
    row = jax.ShapeDtypeStruct((capacity, width + LANES), BF16)
    sent = call(
        partial(dispatch_kernel, tp_count, groups, capacity),
        (row,) * groups,
        (*parts, norm_gain.reshape(1, -1), place, wide, first, route),
        1 << 24,
    )
    arrived = exchange_all(sent, "ep", ep_count, 2)
    made = call(
        partial(expert_kernel, groups, width),
        jax.ShapeDtypeStruct((bins, capacity, part), BF16),
        (*arrived, *weights, *others),
        1 << 30,
        8 << 20,
    )
    homes = [
        [(chip * 2 + core) * tp_count + column for chip in range(groups) for column in range(tp_count)]
        for core in range(2)
    ]
    returned = lax.all_to_all(
        made, ("ep", "tp"), split_axis=0, concat_axis=0, tiled=True, axis_index_groups=homes
    )
    return call(
        restore_kernel, jax.ShapeDtypeStruct(tokens.shape, BF16), (returned, back), 1 << 25
    )


def solution(mesh):
    in_specs = (
        P("ep", "tp"),
        P(),
        P("ep", None, None),
        P("ep", None, None),
        P("ep", None, None),
        P("ep", None),
        P("ep", None),
    )
    group_experts = mesh.shape["tp"] // 2
    pairs = group_experts == 2

    def body(*arrays):
        return (local_pairs if pairs else local_any)(*arrays)

    return jax.shard_map(
        body, mesh=mesh, in_specs=in_specs, out_specs=P("ep", "tp"), check_vma=False
    )
```

```python
from functools import partial

import jax
import jax.numpy as jnp
from jax import lax
from jax.experimental import pallas as pl
from jax.experimental.pallas import tpu as pltpu
from jax.sharding import PartitionSpec as P


F32 = jnp.float32
BF16 = jnp.bfloat16
LANES = 128
VMEM = pl.BlockSpec(memory_space=pltpu.VMEM)


def slot_numbers(block_ids, experts):
    flat_ids = block_ids.reshape(-1)
    hit_table = (flat_ids[:, None] == jnp.arange(experts, dtype=jnp.int32)[None, :]).astype(
        jnp.int32
    )
    earlier = jnp.cumsum(hit_table, axis=0) - hit_table
    return (flat_ids, jnp.sum(earlier * hit_table, axis=1))


def placement_matrix(flat_ids, slot_index, experts, capacity):
    target = (flat_ids * capacity + slot_index).reshape(-1, 2)
    slot_rows = jnp.arange(experts * capacity, dtype=jnp.int32)[:, None]
    first_hit = (target[:, 0][None, :] == slot_rows).astype(BF16)
    second_hit = (target[:, 1][None, :] == slot_rows).astype(BF16)
    return first_hit + second_hit


def expert_apply(row_data, gate_weight, up_weight, down_weight):
    shape_in = row_data.shape
    flat_rows = row_data.reshape(-1, shape_in[-1])
    gate_part = jnp.dot(flat_rows, gate_weight[0], preferred_element_type=F32)
    up_part = jnp.dot(flat_rows, up_weight[0], preferred_element_type=F32)
    hidden = (jax.nn.silu(gate_part) * up_part).astype(BF16)
    produced = jnp.dot(hidden, down_weight[0], preferred_element_type=F32).astype(BF16)
    return produced.reshape(shape_in[:-1] + (produced.shape[-1],))


def local_any(tokens, norm_gain, gate_weight, up_weight, down_weight, expert_ids, route_weight):
    tp_count = lax.axis_size("tp")
    experts = lax.axis_size("ep") * gate_weight.shape[0]
    model_width = gate_weight.shape[1]
    group_rows = tokens.shape[0]
    block_rows = group_rows // tp_count
    capacity = 4 * block_rows // experts
    tp_index = lax.axis_index("tp")
    apply_experts = partial(
        expert_apply, gate_weight=gate_weight, up_weight=up_weight, down_weight=down_weight
    )
    full_rows = lax.all_to_all(tokens, "tp", split_axis=0, concat_axis=1, tiled=True)
    block_ids = lax.dynamic_slice_in_dim(expert_ids, tp_index * block_rows, block_rows, 0)
    block_weight = lax.dynamic_slice_in_dim(route_weight, tp_index * block_rows, block_rows, 0)
    widened = full_rows.astype(F32)
    mean_square = jnp.mean(widened * widened, axis=-1, keepdims=True)
    normed = (widened * lax.rsqrt(mean_square + 1e-06) * norm_gain).astype(BF16)
    flat_ids, slot_index = slot_numbers(block_ids, experts)
    placing = placement_matrix(flat_ids, slot_index, experts, capacity)
    outgoing = jnp.dot(placing, normed, preferred_element_type=F32).astype(BF16)
    outgoing = outgoing.reshape(experts, capacity, model_width)
    produced = apply_experts(
        lax.all_to_all(outgoing, "ep", split_axis=0, concat_axis=0, tiled=True)
    )
    returned = lax.all_to_all(produced, "ep", split_axis=0, concat_axis=0, tiled=True)
    picked = jnp.take(returned.reshape(-1, model_width), flat_ids * capacity + slot_index, axis=0)
    weighted = picked.astype(F32) * block_weight.reshape(-1)[:, None]
    mixed_rows = weighted.reshape(block_rows, 2, model_width).sum(axis=1).astype(BF16)
    return lax.all_to_all(mixed_rows, "tp", split_axis=1, concat_axis=0, tiled=True)


def pause_kernel(out_ref):
    out_ref[...] = jnp.zeros_like(out_ref)


def code_of(place, first, route, core):
    mine = (first & 1) == core
    lane = lax.broadcasted_iota(jnp.int32, (place.shape[0], LANES), 1)
    code = jnp.zeros(lane.shape, F32)
    for which in range(2):
        row = jnp.where(mine, route[which : which + 1], route[1 - which : 2 - which])
        rest = jnp.sum(place * row, axis=1, keepdims=True)
        for part in range(3):
            piece = rest.astype(BF16).astype(F32)
            rest = rest - piece
            code = jnp.where(lane == 3 * which + part, piece, code)
    return code


def dispatch_kernel(
    groups, capacity, block, order, pause_ref, tokens_ref, ids_ref, route_ref, out_ref, back_ref
):
    core = lax.axis_index("ep") % 2
    rows, width = tokens_ref.shape
    columns = rows // block
    first = ids_ref[0:1, :]
    bin_of = (first >> 1) * columns + lax.broadcasted_iota(jnp.int32, (1, rows), 1) // block
    bins = groups * columns
    hot = bin_of == lax.broadcasted_iota(jnp.int32, (bins, rows), 0)
    before = lax.broadcasted_iota(jnp.int32, (rows, rows), 0) < lax.broadcasted_iota(
        jnp.int32, (rows, rows), 1
    )
    ahead = jnp.dot(
        hot.astype(F32).astype(BF16), before.astype(F32).astype(BF16), preferred_element_type=F32
    )
    rank = jnp.sum(jnp.where(hot, ahead, 0.0), axis=0, keepdims=True)
    at = rank == lax.broadcasted_iota(jnp.int32, (capacity, rows), 0).astype(F32)
    place = jnp.concatenate(
        [jnp.where(at & (bin_of == n), 1.0, 0.0) for n in order], axis=0
    )
    placed = jnp.dot(
        place.astype(BF16), tokens_ref[...], preferred_element_type=F32
    ).astype(BF16)
    code = code_of(place, first, route_ref[...], core)
    turned = pltpu.roll(code, 8, 1)
    tiles = width // LANES
    half = capacity // 2
    for n in range(bins):
        low = n * capacity
        for t in range(tiles):
            out_ref[n, t * capacity : (t + 1) * capacity, :] = placed[
                low : low + capacity, t * LANES : (t + 1) * LANES
            ]
        out_ref[n, tiles * capacity :, :] = (
            code[low : low + half] + turned[low + half : low + capacity]
        ).astype(BF16)
    back_ref[...] = place.T.astype(BF16)


def expert_kernel(groups, order, capacity, arrived_ref, gain_ref, *refs):
    weights, out_ref = refs[:6], refs[6]
    part = out_ref.shape[2]
    columns = len(order) // groups
    width = columns * part
    tiles = part // LANES

    def source(chip, column):
        return order.index(chip * columns + column)

    pieces = [
        jnp.concatenate(
            [
                arrived_ref[source(z, n // tiles), n % tiles * capacity : (n % tiles + 1) * capacity, :]
                for z in range(groups)
            ],
            axis=0,
        ).astype(F32)
        for n in range(width // LANES)
    ]
    square = sum(p * p for p in pieces)
    scale = lax.rsqrt(jnp.sum(square, axis=1, keepdims=True) / width + 1e-06)
    x = jnp.concatenate(
        [
            (p * scale * gain_ref[:, n * LANES : (n + 1) * LANES]).astype(BF16)
            for n, p in enumerate(pieces)
        ],
        axis=1,
    )
    hidden, scales = [], []
    for which in range(2):
        gate = jnp.dot(x, weights[3 * which][0], preferred_element_type=F32)
        up = jnp.dot(x, weights[3 * which + 1][0], preferred_element_type=F32)
        hidden.append((gate / (1.0 + jnp.exp(-gate)) * up).astype(BF16))
        columns_of = []
        for z in range(groups):
            code = arrived_ref[source(z, 0), tiles * capacity :, :].astype(F32)
            for lane in (3 * which, 8 + 3 * which):
                columns_of.append(
                    code[:, lane : lane + 1] + code[:, lane + 1 : lane + 2] + code[:, lane + 2 : lane + 3]
                )
        scales.append(jnp.concatenate(columns_of, axis=0))
    for n in range(columns):
        total = None
        for which in range(2):
            down = weights[3 * which + 2][0, :, n * part : (n + 1) * part]
            made = jnp.dot(hidden[which], down, preferred_element_type=F32).astype(BF16)
            term = made.astype(F32) * scales[which]
            total = term if total is None else total + term
        mixed = total.astype(BF16)
        for z in range(groups):
            out_ref[source(z, n)] = mixed[z * capacity : (z + 1) * capacity]


def restore_kernel(rows_ref, back_ref, out_ref):
    rows = rows_ref[...].reshape(-1, rows_ref.shape[-1])
    out_ref[...] = jnp.dot(back_ref[...], rows, preferred_element_type=F32).astype(BF16)


def call(kernel, outs, args, flops, limit=4 << 20, scratch=()):
    return pl.pallas_call(
        kernel,
        out_shape=outs,
        in_specs=[VMEM] * len(args),
        out_specs=jax.tree.map(lambda _: VMEM, outs),
        scratch_shapes=scratch,
        compiler_params=pltpu.CompilerParams(vmem_limit_bytes=limit),
        cost_estimate=pl.CostEstimate(flops=flops, bytes_accessed=1 << 20, transcendentals=0),
    )(*args)


def peer_order(peers):
    spread = [11, 10, 1, 3, 8, 9, 6, 4, 15, 5, 2, 13, 14, 7, 12, 0]
    return spread if len(spread) == peers else list(range(peers))


def local_pairs(tokens, norm_gain, gate_weight, up_weight, down_weight, expert_ids, route_weight):
    tp_count = lax.axis_size("tp")
    ep_count = lax.axis_size("ep")
    groups = ep_count // 2
    all_rows, part = tokens.shape
    block = all_rows // tp_count
    capacity = 4 * block // ep_count
    bins = groups * tp_count
    order = peer_order(bins)
    homes = [
        [(n // tp_count * 2 + core) * tp_count + n % tp_count for n in order] for core in range(2)
    ]

    def trade(array):
        return lax.all_to_all(
            array, ("ep", "tp"), split_axis=0, concat_axis=0, tiled=True, axis_index_groups=homes
        )

    pause = call(pause_kernel, jax.ShapeDtypeStruct((8, LANES), F32), (), 1 << 33)
    weights = (gate_weight, up_weight, down_weight)
    others = []
    for w in weights:
        others.append(lax.ppermute(w, "ep", [(i, i ^ 1) for i in range(ep_count)]))
    sent, back = call(
        partial(dispatch_kernel, groups, capacity, block, order),
        (
            jax.ShapeDtypeStruct((bins, part // LANES * capacity + capacity // 2, LANES), BF16),
            jax.ShapeDtypeStruct((all_rows, bins * capacity), BF16),
        ),
        (pause, tokens, expert_ids.T, route_weight.T),
        1 << 33,
        8 << 20,
    )
    made = call(
        partial(expert_kernel, groups, order, capacity),
        jax.ShapeDtypeStruct((bins, capacity, part), BF16),
        (trade(sent), norm_gain.reshape(1, -1), *weights, *others),
        1 << 30,
        8 << 20,
    )
    return call(
        restore_kernel, jax.ShapeDtypeStruct(tokens.shape, BF16), (trade(made), back), 1 << 25
    )


def solution(mesh):
    in_specs = (
        P("ep", "tp"),
        P(),
        P("ep", None, None),
        P("ep", None, None),
        P("ep", None, None),
        P("ep", None),
        P("ep", None),
    )
    group_experts = mesh.shape["tp"] // 2
    pairs = group_experts == 2

    def body(*arrays):
        return (local_pairs if pairs else local_any)(*arrays)

    return jax.shard_map(
        body, mesh=mesh, in_specs=in_specs, out_specs=P("ep", "tp"), check_vma=False
    )
```
